32 devices in a mesh: ep: 4 (over z), tp: 8 (over y, x, core).
Axes of the slice: x: 2, y: 2, z: 4, core: 2. Of those that a mesh axis runs over, the one named last changes fastest.
Arguments:
- tokens: bfloat16 [672, 2048], P('ep', 'tp'), may hold values from -540 to 540
- norm_gain: float32 [2048], P('tp'), may hold values from 0.1 to 1.9
- chosen: int32 [4, 504], P('ep'), may hold values from 0 to 671, as said below
- affinity: float32 [4, 504], P('ep'), may hold values from 0.1 to 1
- w_gate: bfloat16 [4, 2048, 8192], P('ep', None, 'tp'), may hold values from -0.125 to 0.125
- w_up: bfloat16 [4, 2048, 8192], P('ep', None, 'tp'), may hold values from -0.125 to 0.125
- w_down: bfloat16 [4, 8192, 2048], P('ep', 'tp'), may hold values from -0.0625 to 0.0625
Outputs:
- expert_mix: bfloat16 [672, 2048], P('ep', 'tp')
The draws below stay inside these ranges and needn't reach their ends.
Inputs may be any that keep to these rules, and one draw needn't show every extreme that they name: `chosen`: each expert's 504 token numbers are distinct. Among one expert's choices at most 168 are tokens of one index of ep, and that bound is reached in every draw.
All inputs are finite; a program needn't handle non-finite values.
Results may differ from the reference program's by a relative error of at most 0.025.
Values may be sent and summed in bfloat16 or wider, within the bound.
A program may use at most 64 MiB of HBM per device.

```python
import math
import jax
import jax.numpy as jnp
from jax import lax

D = 2048
FF = 8192
TOK_DEV = 168
TOKENS = 672
EXPERTS = 4
CHOSEN = 504
MOST = 168
N_TP = 8


def draw_tokens(key, part):
    key_noise, key_cols, key_rows = jax.random.split(key, 3)
    col_scale = 6.0 ** (jnp.arange(D, dtype=jnp.float32) / (D - 1))
    col_scale = col_scale * jax.random.uniform(key_cols, (D,), jnp.float32, 0.5, 1.5)
    row_scale = jnp.exp(jax.random.uniform(key_rows, (TOKENS, 1), jnp.float32, 0.0, math.log(10.0)))
    noise = jnp.clip(jax.random.normal(key_noise, (TOKENS, D), jnp.float32), -6.0, 6.0)
    return (noise * col_scale[None, :] * row_scale).astype(jnp.bfloat16)


def draw_chosen(key, part):

    def pick_expert(expert):
        expert_key = jax.random.fold_in(key, expert)
        key_raw, key_full = jax.random.split(expert_key, 2)
        raw_score = jax.random.randint(key_raw, (EXPERTS, TOK_DEV), 0, 32768)
        local_id = jnp.arange(TOK_DEV, dtype=jnp.int32)[None, :]
        source = jnp.arange(EXPERTS, dtype=jnp.int32)[:, None]
        global_id = source * TOK_DEV + local_id
        keyed_score = raw_score * TOK_DEV + local_id
        ranked = jnp.argsort(jnp.argsort(-keyed_score, axis=1), axis=1)
        allowed = ranked < MOST
        full_source = jax.random.randint(key_full, (), 0, EXPERTS)
        before = (expert + EXPERTS - 1) % EXPERTS
        across = (expert + EXPERTS // 2) % EXPERTS
        extra_score = jnp.where(source == full_source, 2, 0)
        extra_score = extra_score + jnp.where(((source == before) | (source == across)) & (ranked == 0), 4, 0)
        priority = allowed.astype(jnp.int32) * (extra_score + 1) * (1 << 27) + raw_score * TOKENS + global_id
        return lax.top_k(priority.reshape(-1), CHOSEN)[1].astype(jnp.int32)
    from_experts = jax.vmap(pick_expert)(jnp.arange(EXPERTS, dtype=jnp.int32))
    return from_experts.astype(jnp.int32)


def levels(rng, dims, cuts, least, high):
    factor_of, own = 1.0, jax.random.fold_in(rng, 6)
    for position, shards_of in cuts:
        draws = jnp.exp(jax.random.uniform(jax.random.fold_in(own, position), (shards_of,), jnp.float32, least / len(cuts), high / len(cuts)))
        factor_of = factor_of * jnp.repeat(draws, dims[position] // shards_of).reshape([-1 if axis == position else 1 for axis in range(len(dims))])
    return factor_of


def bell_draw(rng, shape, deviation, reach, shards=(), held_as=jnp.bfloat16):
    drawn = deviation * jax.random.normal(rng, shape, jnp.float32)
    if shards:
        drawn = drawn * levels(rng, shape, shards, -0.22, 0.18)
    return jnp.clip(drawn, -reach, reach).astype(held_as)


def setup_inputs(seed: int = 0) -> dict:
    arg_keys = jax.random.split(jax.random.key(seed), 8)
    return {
        "tokens": draw_tokens(jax.random.fold_in(arg_keys[7], 71), 0),
        "norm_gain": jnp.clip(1.0 + 0.18 * jax.random.normal(arg_keys[1], (D,), jnp.float32), 0.1, 1.9),
        "chosen": draw_chosen(jax.random.fold_in(arg_keys[7], 71), 0),
        "affinity": jnp.clip(jnp.exp(math.log(1.0) - 2.3025851 * jax.random.uniform(arg_keys[3], (EXPERTS, CHOSEN), jnp.float32) ** levels(arg_keys[3], (EXPERTS, CHOSEN), ((0, 4),), -0.2, 0.2)), 0.1, 1.0),
        "w_gate": bell_draw(arg_keys[4], (EXPERTS, D, FF), D ** -0.5, 0.125, ((0, 4), (2, 8))),
        "w_up": bell_draw(arg_keys[5], (EXPERTS, D, FF), D ** -0.5, 0.125, ((0, 4), (2, 8))),
        "w_down": bell_draw(arg_keys[6], (EXPERTS, FF, D), FF ** -0.5, 0.0625, ((0, 4), (1, 8))),
    }


EPS = 1e-06

def reference(tokens, norm_gain, chosen, affinity, w_gate, w_up, w_down):
    floats = tokens.astype(jnp.float32)
    mean_square = lax.optimization_barrier(jnp.mean(floats * floats, axis=1))
    normed = (floats * lax.rsqrt(mean_square + EPS)[:, None] * norm_gain[None, :]).astype(jnp.bfloat16)

    def single(packed):
        index_row, weight_row, gate_weights, up_weights, down_weights = packed
        picked = normed[index_row]
        gate = jnp.dot(picked, gate_weights, preferred_element_type=jnp.float32)
        upward = jnp.dot(picked, up_weights, preferred_element_type=jnp.float32)
        hidden = (jax.nn.silu(gate) * upward).astype(jnp.bfloat16)
        blocks = hidden.reshape(hidden.shape[0], N_TP, FF // N_TP).astype(jnp.float32)
        down_blocks = down_weights.reshape(N_TP, FF // N_TP, D).astype(jnp.float32)
        partial_value = jnp.einsum('cnf,nfd->ncd', blocks, down_blocks).astype(jnp.bfloat16)
        partial_value = lax.optimization_barrier(partial_value)
        summed = lax.optimization_barrier(jnp.sum(partial_value.astype(jnp.float32), axis=0))
        return (summed * weight_row[:, None]).astype(jnp.bfloat16)
    outputs = lax.map(single, (chosen, affinity, w_gate, w_up, w_down))
    total = jnp.zeros((TOKENS, D), jnp.float32)
    total = total.at[chosen.reshape(-1)].add(outputs.reshape(-1, D).astype(jnp.float32))
    return total.astype(jnp.bfloat16)
```

```python
import functools

import jax
import jax.numpy as jnp
from jax import lax
from jax.experimental import pallas as pl
from jax.experimental.pallas import tpu as pltpu
from jax.sharding import PartitionSpec as P

MESH = pl.DeviceIdType.MESH
VMEM_BYTES = 67_043_328
LANES = 128
SHARES = (1, 1, 1, 1)
AG_ACROSS = (0, 1, 2, 3)
SUM_ACROSS = (0, 1, 2, 3)


def kernel(
    ep, tp, sizes,
    tok_hbm, gain_hbm, chosen_hbm, aff_hbm, wg_hbm, wu_hbm, wd_hbm,
    out,
    tok, gain, chosen, aff, wg, wu, wd, full, hidden, part, got1, got2, sums_even, own, weighted,
    near, back, got_back, chosen_row, aff_row, slot_row, slot_col,
    aff_col, square_row, keep, in_sem, w_sem, s_send, s_recv, z_send, z_recv, ag_send, ag_recv,
    r1_send, r1_recv, r2_send, r2_recv, b_send, b_recv,
):
    me = lax.axis_index("ep")
    t = lax.axis_index("tp")
    tok_dev, width = tok.shape
    rows = full.shape[1]
    d = wg.shape[0]
    count = chosen.shape[1]
    ff = wg.shape[1]
    chunks = len(sizes)
    starts = [sum(sizes[:c]) for c in range(chunks)]
    ends = [sum(sizes[: c + 1]) for c in range(chunks)]
    f32, bf16 = jnp.float32, jnp.bfloat16
    scope = jax.named_scope

    def flip(m):
        index, bit = t, 1
        while bit <= m:
            if m & bit:
                index = index + bit - 2 * bit * ((t // bit) % 2)
            bit *= 2
        return index

    def cols(m):
        return pl.ds(pl.multiple_of(flip(m) * width, LANES), width)

    def remote(src, dst, send, recv, ep_to, tp_to):
        return pltpu.make_async_remote_copy(
            src_ref=src, dst_ref=dst, send_sem=send, recv_sem=recv,
            device_id=(ep_to, tp_to), device_id_type=MESH,
        )

    def whole(ref, send, recv):
        return remote(ref, ref, send, recv, me, flip(1))

    evens = [6, 2, 4, 0]
    order = list(range(chunks))
    weights = [
        pltpu.make_async_copy(h.at[0], v, w_sem.at[i])
        for i, (h, v) in enumerate(((wg_hbm, wg), (wu_hbm, wu), (wd_hbm, wd)))
    ]
    inputs = [
        pltpu.make_async_copy(h, v, in_sem.at[i])
        for i, (h, v) in enumerate(
            ((tok_hbm, tok), (gain_hbm, gain), (chosen_hbm, chosen), (aff_hbm, aff))
        )
    ]
    for copy in inputs:
        copy.start()

    spare = ep * tok_dev - count
    need = [min(tok_dev, -(-(-(-(ends[c] + spare) // ep)) // 16) * 16) for c in order]
    need[-1] = tok_dev
    least = [starts[c] // ep // 16 * 16 for c in order]
    done = [min(tok_dev, ends[c] // ep // 16 * 16) for c in order]
    done[-1] = tok_dev

    def piece(stops, c):
        start = stops[c - 1] if c else 0
        return pl.ds(start, stops[c] - start)

    barrier = pltpu.get_barrier_semaphore()
    for m in range(1, tp):
        pl.semaphore_signal(barrier, inc=1, device_id=(me, flip(m)), device_id_type=MESH)
    for k in range(1, ep):
        pl.semaphore_signal(
            barrier, inc=1, device_id=(lax.rem(me + k, ep), t), device_id_type=MESH
        )
    with scope("inputs"):
        for copy in inputs:
            copy.wait()
    for copy in weights:
        copy.start()
    with scope("barrier"):
        pl.semaphore_wait(barrier, tp + ep - 2)

    def z_copy(c, k):
        rows_c = piece(need, c)
        return remote(
            tok.at[rows_c, :], near.at[k, rows_c, :], z_send.at[0], z_recv.at[c],
            lax.rem(me + k, ep), t,
        )

    def z_start(c):
        if piece(need, c).size:
            for k in range(1, ep):
                z_copy(c, k).start()

    z_start(0)

    with scope("index"):
        chosen_row[...] = jnp.full(chosen_row.shape, -1.0, f32)
        aff_row[...] = jnp.zeros(aff_row.shape, f32)
        chosen_row[:, :count] = chosen[...].astype(f32)
        aff_row[:, :count] = aff[...]
        diagonal = lax.broadcasted_iota(jnp.int32, (rows, rows), 0) == lax.broadcasted_iota(
            jnp.int32, (rows, rows), 1
        )
        given = jnp.sum(jnp.where(diagonal, chosen_row[...], 0.0), axis=1, keepdims=True)
        factor = jnp.sum(jnp.where(diagonal, aff_row[...], 0.0), axis=1, keepdims=True)

        owners = [lax.rem(me + q, ep) for q in range(ep)]
        lane = lax.broadcasted_iota(jnp.int32, (rows, tok_dev), 1)
        sub = lax.broadcasted_iota(jnp.int32, (tok_dev, rows), 0)
        taken_row, taken_col, aff_token = [], [], []
        for q in range(ep):
            match = given == (lane + owners[q] * tok_dev).astype(f32)
            taken_row.append(jnp.sum(match.astype(f32), axis=0, keepdims=True))
            aff_token.append(jnp.sum(jnp.where(match, factor, 0.0), axis=0, keepdims=True))
            match = chosen_row[...] == (sub + owners[q] * tok_dev).astype(f32)
            taken_col.append(jnp.sum(match.astype(f32), axis=1, keepdims=True))
        down_index = lax.broadcasted_iota(jnp.int32, (tok_dev, tok_dev), 0) * ep
        across_index = lax.broadcasted_iota(jnp.int32, (tok_dev, tok_dev), 1) * ep
        place_all = lax.broadcasted_iota(jnp.int32, (rows, tok_dev), 0).astype(f32)
        factor_sum = jnp.zeros((rows, tok_dev), f32)
        for q in range(ep):
            ahead = jnp.zeros((tok_dev, tok_dev), f32)
            above = jnp.zeros((tok_dev, tok_dev), f32)
            for p in range(ep):
                ahead = ahead + jnp.where(
                    down_index + owners[p] < across_index + owners[q], taken_col[p], 0.0
                )
                above = above + jnp.where(
                    across_index + owners[p] < down_index + owners[q], taken_row[p], 0.0
                )
            slot_row[q] = jnp.where(
                taken_row[q] > 0, jnp.sum(ahead, axis=0, keepdims=True), -1.0
            )
            slot_col[q] = jnp.where(
                taken_col[q] > 0, jnp.sum(above, axis=1, keepdims=True), -1.0
            )
            factor_sum = factor_sum + jnp.where(place_all == slot_row[q], aff_token[q], 0.0)
        aff_col[...] = jnp.sum(factor_sum, axis=1, keepdims=True)

    def span(c):
        return pl.ds(starts[c], sizes[c])

    def part_rows(c, part_of):
        half = sizes[c] // 2
        return pl.ds(starts[c] + part_of * half, half)

    routes = {
        1: (0, None, 1), 2: (0, None, 2), 4: (0, None, 4),
        3: (2, None, 1), 6: (2, 0, 4), 5: (4, None, 1), 8: (4, 1, 2),
        7: (6, 0, 1), 9: (6, 1, 1),
    }

    across = {
        1: (0, None, 1), 2: (0, None, 2), 4: (0, None, 4), 6: (0, None, 6),
        3: (2, None, 1), 5: (4, None, 1), 7: (6, None, 1),
    }
    ag_slot = {2: 1, 4: 2, 6: 3, 8: 4, 1: 0, 3: 0, 5: 0, 7: 0, 9: 0}

    def route(c, s):
        return (across if c in AG_ACROSS else routes)[s]

    def ag_block(c, m, part_of):
        return full.at[flip(m), span(c) if part_of is None else part_rows(c, part_of), :]

    def ag_copy(c, s):
        m, part_of, to = route(c, s)
        block = ag_block(c, m, part_of)
        return remote(block, block, ag_send.at[0], ag_recv.at[c, ag_slot[s]], me, flip(to))

    def ag_wait(c, s):
        m, part_of, to = route(c, s)
        block = ag_block(c, m ^ to, part_of)
        whole(block, ag_send.at[0], ag_recv.at[c, ag_slot[s]]).wait_recv()

    def square_copy(c, m):
        return remote(
            square_row.at[c, 0], square_row.at[c, m], s_send.at[0], s_recv.at[c], me, flip(m)
        )

    def pick(c):
        low, high, size = least[c], need[c], sizes[c]
        place = (
            lax.broadcasted_iota(jnp.int32, (size, high - low), 0) + starts[c]
        ).astype(f32)
        hots = []
        for k in range(ep):
            q = (ep - k) % ep
            hots.append((place == slot_row[q, :, low:high]).astype(f32).astype(bf16))
        with scope(f"zwait{c}"):
            if piece(need, c).size:
                rows_c = piece(need, c)
                whole(near.at[1:, rows_c, :], z_send.at[0], z_recv.at[c]).wait_recv()
        with scope(f"pick{c}"):
            total = jnp.zeros((size, width), f32)
            for k in range(ep):
                block = tok[low:high, :] if k == 0 else near[k, low:high, :]
                total = total + jnp.dot(hots[k], block, preferred_element_type=f32)
            full[t, span(c), :] = (total * gain[...]).astype(bf16)
            for s in (6, 2, 4, 1) if c in AG_ACROSS else (2, 4, 1):
                ag_copy(c, s).start()
            diagonal = lax.broadcasted_iota(jnp.int32, (size, size), 0) == (
                lax.broadcasted_iota(jnp.int32, (size, size), 1)
            )
            squares = jnp.sum(total * total, axis=1, keepdims=True)
            square_row[c, 0, :, :size] = jnp.sum(
                jnp.where(diagonal, squares, 0.0), axis=0, keepdims=True
            )
            for m in range(1, tp):
                square_copy(c, m).start()

    def forward(c, stages):
        with scope(f"fwd{c}_{stages[0][0]}"):
            for s, onward in stages:
                ag_wait(c, s)
                for after in onward:
                    ag_copy(c, after).start()

    first = ((2, (6, 3)), (4, (8, 5)))
    second = ((6, (7,)), (8, (9,)))

    sums = (
        (2, 0, 0, 2), (4, 1, 0, 4), (6, 0, 1, 2), (6, 1, 1, 4), (4, 0, 2, 4), (2, 1, 2, 2),
    )

    def r1_copy(c, i):
        return remote(
            part.at[2 * i + 1, span(c), :], got1.at[i, span(c), :],
            r1_send.at[0], r1_recv.at[c, int(i == 3)], me, flip(1),
        )

    def r2_copy(c, s):
        m, part_of, slot, to = sums[s]
        rows_h = part_rows(c, part_of)
        return remote(
            part.at[m, rows_h, :], got2.at[slot, rows_h, :],
            r2_send.at[0], r2_recv.at[c, {2: 1, 3: 2}.get(s, 0)], me, flip(to),
        )

    tile = min(ff, 256)

    def gate_up(c):
        with scope(f"agwait{c}"):
            whole(full.at[: tp // 2, span(c), :], ag_send.at[0], ag_recv.at[c, 0]).wait_recv()
            whole(square_row.at[c, 1:], s_send.at[0], s_recv.at[c]).wait_recv()
        with scope(f"gateup{c}"):
            size = sizes[c]
            diagonal = lax.broadcasted_iota(jnp.int32, (size, size), 0) == (
                lax.broadcasted_iota(jnp.int32, (size, size), 1)
            )
            squares = square_row[c, 0, :, :size]
            for m in range(1, tp):
                squares = squares + square_row[c, m, :, :size]
            squares = jnp.sum(jnp.where(diagonal, squares, 0.0), axis=1, keepdims=True)
            scale = lax.rsqrt(squares / d + EPS)
            for j in range(ff // tile):
                units = slice(j * tile, (j + 1) * tile)
                gate = jnp.zeros((sizes[c], tile), f32)
                upward = jnp.zeros((sizes[c], tile), f32)
                for b in range(tp):
                    at = slice(b * width, (b + 1) * width)
                    gate = gate + jnp.dot(
                        full[b, span(c), :], wg[at, units], preferred_element_type=f32
                    )
                    upward = upward + jnp.dot(
                        full[b, span(c), :], wu[at, units], preferred_element_type=f32
                    )
                gate, upward = gate * scale, upward * scale
                hidden[c % 2, : sizes[c], units] = (
                    gate / (1.0 + jnp.exp(-gate)) * upward
                ).astype(bf16)

    def down(c):
        def block(m):
            return jnp.dot(
                hidden[c % 2, : sizes[c], :], wd[:, cols(m)], preferred_element_type=f32
            )

        with scope(f"odd{c}"):
            for m in evens:
                part[m + 1, span(c), :] = block(m + 1).astype(bf16)
            if c == chunks - 1:
                for m in evens:
                    r1_copy(c, m // 2).start()
        with scope(f"even{c}"):
            for m in evens:
                sums_even[m // 2, span(c), :] = block(m)
            if c < chunks - 1:
                for m in evens:
                    r1_copy(c, m // 2).start()

    def sum_copy(c, m):
        return remote(
            part.at[m, span(c), :], got2.at[m // 2 - 1, span(c), :],
            r2_send.at[0], r2_recv.at[c, 0], me, flip(m),
        )

    def reduce(c):
        half = sizes[c] // 2
        with scope(f"reduce{c}"):
            for m in evens:
                if m == 6:
                    whole(got1.at[3, span(c), :], r1_send.at[0], r1_recv.at[c, 1]).wait_recv()
                elif m == 2:
                    whole(got1.at[:3, span(c), :], r1_send.at[0], r1_recv.at[c, 0]).wait_recv()
                mine = sums_even[m // 2, span(c), :] + got1[m // 2, span(c), :].astype(f32)
                if m and c in SUM_ACROSS:
                    part[m, span(c), :] = mine.astype(bf16)
                    sum_copy(c, m).start()
                elif m == 6:
                    part[6, span(c), :] = mine.astype(bf16)
                    r2_copy(c, 2).start()
                    r2_copy(c, 3).start()
                elif m:
                    part_of = 0 if m == 2 else 1
                    sent, kept = part_of * half, (1 - part_of) * half
                    part[m, part_rows(c, part_of), :] = mine[sent : sent + half].astype(bf16)
                    r2_copy(c, part_of).start()
                    keep[part_rows(c, 1 - part_of), :] = mine[kept : kept + half]
                else:
                    own[span(c), :] = mine

    def relay(c):
        if c in SUM_ACROSS:
            return
        with scope(f"relay{c}"):
            for s, m, part_of in ((2, 4, 0), (3, 2, 1)):
                rows_h = part_rows(c, part_of)
                r2_copy(c, s).wait_recv()
                part[m, rows_h, :] = (
                    keep[rows_h, :] + got2[1, rows_h, :].astype(f32)
                ).astype(bf16)
                r2_copy(c, s + 2).start()

    def finish(c):
        rows_c = piece(done, c)
        low = max(0, (starts[c] - spare) // LANES * LANES)
        hots = []
        if rows_c.size:
            place = lax.broadcasted_iota(jnp.int32, (rows_c.size, ends[c] - low), 1) + low
            for k in range(ep):
                hots.append(
                    (slot_col[k, rows_c, :] == place.astype(f32)).astype(f32).astype(bf16)
                )
        with scope(f"sumwait{c}"):
            whole(got2.at[: 3 if c in SUM_ACROSS else 2, span(c), :], r2_send.at[0], r2_recv.at[c, 0]).wait_recv()
        with scope(f"finish{c}"):
            at = span(c)
            total = own[at, :] + got2[0, at, :].astype(f32) + got2[2, at, :].astype(f32)
            if c in SUM_ACROSS:
                total = total + got2[1, at, :].astype(f32)
            weighted[at, :] = (total * aff_col[at, :]).astype(bf16)
            if rows_c.size:
                for k in range(ep):
                    back[k, rows_c, :] = jnp.dot(
                        hots[k], weighted[low : ends[c], :], preferred_element_type=f32
                    ).astype(bf16)
                for k in range(1, ep):
                    back_copy(c, k).start()

    def back_copy(c, k):
        rows_c = piece(done, c)
        return remote(
            back.at[k, rows_c, :], got_back.at[k, rows_c, :], b_send.at[0], b_recv.at[c],
            lax.rem(me + k, ep), t,
        )

    def mix(c):
        if piece(done, c).size:
            with scope(f"mix{c}"):
                rows_c = piece(done, c)
                total = back[0, rows_c, :].astype(f32)
                whole(got_back.at[1:, rows_c, :], b_send.at[0], b_recv.at[c]).wait_recv()
                for k in range(1, ep):
                    total = total + got_back[k, rows_c, :].astype(f32)
                out[rows_c, :] = total.astype(bf16)

    def fwd_a(c):
        forward(c, ((2, (3,)), (4, (5,))) if c in AG_ACROSS else first)

    def fwd_b(c):
        forward(c, ((6, (7,)),) if c in AG_ACROSS else second)

    def wait_weights(c):
        with scope("wwait"):
            weights[c].wait()

    steps = {
        "pick": pick, "A": fwd_a, "B": fwd_b, "gu": gate_up, "dn": down, "red": reduce,
        "rel": relay, "fin": finish, "mix": mix, "w": wait_weights, "z": z_start,
    }
    for name, c in ORDER:
        steps[name](c)

    with scope("tail"):
        for ref, send, recv in (
            (square_row.at[:, 1:], s_send, s_recv),
            (near.at[1:], z_send, s_recv),
            (got_back.at[1:], b_send, s_recv),
            (full.at[: tp - 1], ag_send, s_recv),
            (got2, r2_send, s_recv),
            (got1, r1_send, s_recv),
        ):
            whole(ref, send.at[0], recv.at[0]).wait_send()


ORDER = (
    ("z", 1), ("z", 2), ("z", 3), ("pick", 0), ("pick", 1), ("A", 0), ("B", 0), ("pick", 2),
    ("pick", 3), ("w", 0), ("w", 1), ("gu", 0), ("A", 1), ("B", 1), ("w", 2), ("dn", 0), ("A", 2),
    ("B", 2), ("gu", 1), ("red", 0), ("A", 3), ("B", 3), ("dn", 1), ("gu", 2), ("red", 1),
    ("rel", 0), ("dn", 2), ("gu", 3), ("red", 2), ("rel", 1), ("dn", 3), ("fin", 0), ("red", 3),
    ("rel", 2), ("fin", 1), ("rel", 3), ("fin", 2), ("fin", 3), ("mix", 0), ("mix", 1), ("mix", 2),
    ("mix", 3),
)


def fused(ep, tp, tokens, norm_gain, chosen, affinity, w_gate, w_up, w_down):
    tok_dev, width = tokens.shape
    d, ff = w_gate.shape[1:]
    count = chosen.shape[1]
    step = 32 * sum(SHARES)
    rows = -(-count // step) * step
    sizes = tuple(rows // sum(SHARES) * share for share in SHARES)
    largest = max(sizes)
    f32, bf16 = jnp.float32, jnp.bfloat16
    vmem = pl.BlockSpec(memory_space=pltpu.VMEM)
    hbm = pl.BlockSpec(memory_space=pl.ANY)
    dma = pltpu.SemaphoreType.DMA
    return pl.pallas_call(
        functools.partial(kernel, ep, tp, sizes),
        out_shape=pltpu.VMEM((tok_dev, width), bf16),
        in_specs=[hbm] * 7,
        out_specs=vmem,
        scratch_shapes=[
            pltpu.VMEM((tok_dev, width), bf16),
            pltpu.VMEM((1, width), f32),
            pltpu.VMEM((1, count), jnp.int32),
            pltpu.VMEM((1, count), f32),
            pltpu.VMEM((d, ff), bf16),
            pltpu.VMEM((d, ff), bf16),
            pltpu.VMEM((ff, d), bf16),
            pltpu.VMEM((tp, rows, width), bf16),
            pltpu.VMEM((2, largest, ff), bf16),
            pltpu.VMEM((tp, rows, width), bf16),
            pltpu.VMEM((tp // 2, rows, width), bf16),
            pltpu.VMEM((3, rows, width), bf16),
            pltpu.VMEM((tp // 2, rows, width), f32),
            pltpu.VMEM((rows, width), f32),
            pltpu.VMEM((rows, width), bf16),
            pltpu.VMEM((ep, tok_dev, width), bf16),
            pltpu.VMEM((ep, tok_dev, width), bf16),
            pltpu.VMEM((ep, tok_dev, width), bf16),
            pltpu.VMEM((1, rows), f32),
            pltpu.VMEM((1, rows), f32),
            pltpu.VMEM((ep, 1, tok_dev), f32),
            pltpu.VMEM((ep, tok_dev, 1), f32),
            pltpu.VMEM((rows, 1), f32),
            pltpu.VMEM((len(SHARES), tp, 1, -(-largest // LANES) * LANES), f32),
            pltpu.VMEM((rows, width), f32),
            dma((4,)),
            dma((3,)),
            dma((1,)),
            dma((len(SHARES),)),
            dma((1,)),
            dma((len(SHARES),)),
            dma((1,)),
            dma((len(SHARES), 5)),
            dma((1,)),
            dma((len(SHARES), 2)),
            dma((1,)),
            dma((len(SHARES), 3)),
            dma((1,)),
            dma((len(SHARES),)),
        ],
        compiler_params=pltpu.CompilerParams(
            collective_id=0, has_side_effects=True, vmem_limit_bytes=VMEM_BYTES - 2**20
        ),
    )(tokens, norm_gain[None, :], chosen, affinity, w_gate, w_up, w_down)


EPS = 1e-06


def plain(tokens, norm_gain, chosen, affinity, w_gate, w_up, w_down):
    tok_dev, width_part = tokens.shape
    ep_count = lax.axis_size("ep")
    floats = tokens.astype(jnp.float32)
    square_sum = lax.psum(jnp.sum(floats * floats, axis=1), "tp")
    normed = (floats * lax.rsqrt(square_sum / w_gate.shape[1] + EPS)[:, None] * norm_gain[None, :]).astype(
        jnp.bfloat16
    )
    own_choice = chosen[0]
    chosen_count = own_choice.shape[0]
    bound_rows = min(tok_dev, 2 * chosen_count // ep_count)
    slot_ids = jnp.arange(bound_rows, dtype=jnp.int32)
    positions = jnp.arange(chosen_count, dtype=jnp.int32)
    every_token = lax.all_gather(normed, "ep", axis=0, tiled=True)
    picked = every_token[own_choice]
    piece = lax.all_gather(picked, "tp", axis=1, tiled=True)
    gate_rows = w_gate[0]
    up_rows = w_up[0]
    gate = jnp.dot(piece, gate_rows, preferred_element_type=jnp.float32)
    upward = jnp.dot(piece, up_rows, preferred_element_type=jnp.float32)
    hidden = (jax.nn.silu(gate) * upward).astype(jnp.bfloat16)
    columns = w_down[0]
    summed = lax.psum_scatter(
        lax.dot_general(
            columns, hidden, (((0,), (1,)), ((), ())), preferred_element_type=jnp.float32
        ).astype(jnp.bfloat16),
        "tp",
        scatter_dimension=0,
        tiled=True,
    ).astype(jnp.float32)
    weighted = (summed * affinity[0][None, :]).astype(jnp.bfloat16).T
    owner = own_choice // tok_dev
    owner_local = own_choice - owner * tok_dev
    owner_hot = owner[:, None] == jnp.arange(ep_count, dtype=jnp.int32)[None, :]
    running = jnp.cumsum(owner_hot.astype(jnp.int32), axis=0)
    place = jnp.sum(jnp.where(owner_hot, running, 0), axis=1) - 1
    back_match = owner_hot.T[:, None, :] & (place[None, None, :] == slot_ids[None, :, None])
    back_filled = jnp.any(back_match, axis=2)
    back_pick = jnp.sum(jnp.where(back_match, positions[None, None, :], 0), axis=2)
    back_rows = jnp.where(back_filled[..., None], weighted[back_pick], jnp.zeros((), jnp.bfloat16))
    back_token = jnp.where(back_filled, owner_local[back_pick], tok_dev)
    got_back, got_token = (
        lax.all_to_all(back_rows, "ep", split_axis=0, concat_axis=0, tiled=True),
        lax.all_to_all(back_token, "ep", split_axis=0, concat_axis=0, tiled=True),
    )
    total = jnp.zeros((tok_dev, width_part), jnp.float32)
    total = total.at[got_token.reshape(-1)].add(
        got_back.reshape(-1, width_part).astype(jnp.float32), mode="drop"
    )
    return total.astype(jnp.bfloat16)


def solution(mesh):
    ep, tp = mesh.shape["ep"], mesh.shape["tp"]

    def local(tokens, *rest):
        whole_lanes = tokens.shape[1] % LANES == 0 and rest[3].shape[2] % LANES == 0
        if whole_lanes and tp == 2**3:
            return fused(ep, tp, tokens, *rest)
        return plain(tokens, *rest)

    in_specs = (
        P("ep", "tp"),
        P("tp"),
        P("ep", None),
        P("ep", None),
        P("ep", None, "tp"),
        P("ep", None, "tp"),
        P("ep", "tp", None),
    )
    out_specs = P("ep", "tp")
    return jax.shard_map(local, mesh=mesh, in_specs=in_specs, out_specs=out_specs, check_vma=False)
```

```python
import functools

import jax
import jax.numpy as jnp
from jax import lax
from jax.experimental import pallas as pl
from jax.experimental.pallas import tpu as pltpu
from jax.sharding import PartitionSpec as P

MESH = pl.DeviceIdType.MESH
VMEM_BYTES = 67_043_328
LANES = 128
SHARES = (1, 1, 1, 1)
AG_ACROSS = (0, 1, 2, 3)
SUM_ACROSS = (0, 1, 2, 3)


def kernel(
    ep, tp, sizes,
    tok_hbm, gain_hbm, chosen_hbm, aff_hbm, wg_hbm, wu_hbm, wd_hbm,
    out,
    tok, gain, chosen, aff, wg, wu, wd, full, hidden, part, got1, got2, sums_even, own, weighted,
    near, back, got_back, chosen_row, aff_row, slot_row, slot_col,
    aff_col, square_row, keep, in_sem, w_sem, s_send, s_recv, z_send, z_recv, ag_send, ag_recv,
    r1_send, r1_recv, r2_send, r2_recv, b_send, b_recv,
):
    me = lax.axis_index("ep")
    t = lax.axis_index("tp")
    tok_dev, width = tok.shape
    rows = full.shape[1]
    d = wg.shape[0]
    count = chosen.shape[1]
    ff = wg.shape[1]
    chunks = len(sizes)
    starts = [sum(sizes[:c]) for c in range(chunks)]
    ends = [sum(sizes[: c + 1]) for c in range(chunks)]
    f32, bf16 = jnp.float32, jnp.bfloat16
    scope = jax.named_scope

    def flip(m):
        index, bit = t, 1
        while bit <= m:
            if m & bit:
                index = index + bit - 2 * bit * ((t // bit) % 2)
            bit *= 2
        return index

    def cols(m):
        return pl.ds(pl.multiple_of(flip(m) * width, LANES), width)

    def remote(src, dst, send, recv, ep_to, tp_to):
        return pltpu.make_async_remote_copy(
            src_ref=src, dst_ref=dst, send_sem=send, recv_sem=recv,
            device_id=(ep_to, tp_to), device_id_type=MESH,
        )

    def whole(ref, send, recv):
        return remote(ref, ref, send, recv, me, flip(1))

    evens = [6, 2, 4, 0]
    order = list(range(chunks))
    weights = [
        pltpu.make_async_copy(h.at[0], v, w_sem.at[i])
        for i, (h, v) in enumerate(((wg_hbm, wg), (wu_hbm, wu), (wd_hbm, wd)))
    ]
    inputs = [
        pltpu.make_async_copy(h, v, in_sem.at[i])
        for i, (h, v) in enumerate(
            ((tok_hbm, tok), (gain_hbm, gain), (chosen_hbm, chosen), (aff_hbm, aff))
        )
    ]
    for copy in inputs:
        copy.start()

    spare = ep * tok_dev - count
    need = [min(tok_dev, -(-(-(-(ends[c] + spare) // ep)) // 16) * 16) for c in order]
    need[-1] = tok_dev
    least = [starts[c] // ep // 16 * 16 for c in order]
    done = [min(tok_dev, ends[c] // ep // 16 * 16) for c in order]
    done[-1] = tok_dev

    def piece(stops, c):
        start = stops[c - 1] if c else 0
        return pl.ds(start, stops[c] - start)

    barrier = pltpu.get_barrier_semaphore()
    for m in range(1, tp):
        pl.semaphore_signal(barrier, inc=1, device_id=(me, flip(m)), device_id_type=MESH)
    for k in range(1, ep):
        pl.semaphore_signal(
            barrier, inc=1, device_id=(lax.rem(me + k, ep), t), device_id_type=MESH
        )
    with scope("inputs"):
        for copy in inputs:
            copy.wait()
    for copy in weights:
        copy.start()
    with scope("barrier"):
        pl.semaphore_wait(barrier, tp + ep - 2)

    def z_copy(c, k):
        rows_c = piece(need, c)
        return remote(
            tok.at[rows_c, :], near.at[k, rows_c, :], z_send.at[0], z_recv.at[c],
            lax.rem(me + k, ep), t,
        )

    def farthest_first():
        after, before = ep - 1 - me, me
        longer = (after - before + ep) // ep
        gap = (2 * longer - 1) * (after - before)
        short = (ep - 1 - gap) // 2
        steps = []
        for i in range(ep - 1):
            alone = (gap - 1 - i + ep) // ep
            far = longer * (ep - 1 - i) + (1 - longer) * i
            pair = i - gap
            near_by = me + (1 - 2 * ((pair + 2 * ep) % 2)) * (short - (pair + 2 * ep) // 2 + ep)
            to = alone * far + (1 - alone) * near_by
            steps.append(lax.rem(to - me + ep, ep))
        return steps

    hops = farthest_first()
    hops = hops[:1] + hops[:0:-1]

    def z_start(c):
        if piece(need, c).size:
            for k in hops:
                z_copy(c, k).start()

    z_start(0)

    with scope("index"):
        chosen_row[...] = jnp.full(chosen_row.shape, -1.0, f32)
        aff_row[...] = jnp.zeros(aff_row.shape, f32)
        chosen_row[:, :count] = chosen[...].astype(f32)
        aff_row[:, :count] = aff[...]
        diagonal = lax.broadcasted_iota(jnp.int32, (rows, rows), 0) == lax.broadcasted_iota(
            jnp.int32, (rows, rows), 1
        )
        given = jnp.sum(jnp.where(diagonal, chosen_row[...], 0.0), axis=1, keepdims=True)
        factor = jnp.sum(jnp.where(diagonal, aff_row[...], 0.0), axis=1, keepdims=True)

        owners = [lax.rem(me + q, ep) for q in range(ep)]
        lane = lax.broadcasted_iota(jnp.int32, (rows, tok_dev), 1)
        sub = lax.broadcasted_iota(jnp.int32, (tok_dev, rows), 0)
        taken_row, taken_col, aff_token = [], [], []
        for q in range(ep):
            match = given == (lane + owners[q] * tok_dev).astype(f32)
            taken_row.append(jnp.sum(match.astype(f32), axis=0, keepdims=True))
            aff_token.append(jnp.sum(jnp.where(match, factor, 0.0), axis=0, keepdims=True))
            match = chosen_row[...] == (sub + owners[q] * tok_dev).astype(f32)
            taken_col.append(jnp.sum(match.astype(f32), axis=1, keepdims=True))
        down_index = lax.broadcasted_iota(jnp.int32, (tok_dev, tok_dev), 0) * ep
        across_index = lax.broadcasted_iota(jnp.int32, (tok_dev, tok_dev), 1) * ep
        place_all = lax.broadcasted_iota(jnp.int32, (rows, tok_dev), 0).astype(f32)
        factor_sum = jnp.zeros((rows, tok_dev), f32)
        for q in range(ep):
            ahead = jnp.zeros((tok_dev, tok_dev), f32)
            above = jnp.zeros((tok_dev, tok_dev), f32)
            for p in range(ep):
                ahead = ahead + jnp.where(
                    down_index + owners[p] < across_index + owners[q], taken_col[p], 0.0
                )
                above = above + jnp.where(
                    across_index + owners[p] < down_index + owners[q], taken_row[p], 0.0
                )
            slot_row[q] = jnp.where(
                taken_row[q] > 0, jnp.sum(ahead, axis=0, keepdims=True), -1.0
            )
            slot_col[q] = jnp.where(
                taken_col[q] > 0, jnp.sum(above, axis=1, keepdims=True), -1.0
            )
            factor_sum = factor_sum + jnp.where(place_all == slot_row[q], aff_token[q], 0.0)
        aff_col[...] = jnp.sum(factor_sum, axis=1, keepdims=True)

    def span(c):
        return pl.ds(starts[c], sizes[c])

    def part_rows(c, part_of):
        half = sizes[c] // 2
        return pl.ds(starts[c] + part_of * half, half)

    routes = {
        1: (0, None, 1), 2: (0, None, 2), 4: (0, None, 4),
        3: (2, None, 1), 6: (2, 0, 4), 5: (4, None, 1), 8: (4, 1, 2),
        7: (6, 0, 1), 9: (6, 1, 1),
    }

    across = {
        1: (0, None, 1), 2: (0, None, 2), 4: (0, None, 4), 6: (0, None, 6),
        3: (2, None, 1), 5: (4, None, 1), 7: (6, None, 1),
    }
    ag_slot = {2: 1, 4: 2, 6: 3, 8: 4, 1: 0, 3: 0, 5: 0, 7: 0, 9: 0}

    def route(c, s):
        return (across if c in AG_ACROSS else routes)[s]

    def ag_block(c, m, part_of):
        return full.at[flip(m), span(c) if part_of is None else part_rows(c, part_of), :]

    def ag_copy(c, s):
        m, part_of, to = route(c, s)
        block = ag_block(c, m, part_of)
        return remote(block, block, ag_send.at[0], ag_recv.at[c, ag_slot[s]], me, flip(to))

    def ag_wait(c, s):
        m, part_of, to = route(c, s)
        block = ag_block(c, m ^ to, part_of)
        whole(block, ag_send.at[0], ag_recv.at[c, ag_slot[s]]).wait_recv()

    def square_copy(c, m):
        return remote(
            square_row.at[c, 0], square_row.at[c, m], s_send.at[0], s_recv.at[c], me, flip(m)
        )

    def pick(c):
        low, high, size = least[c], need[c], sizes[c]
        place = (
            lax.broadcasted_iota(jnp.int32, (size, high - low), 0) + starts[c]
        ).astype(f32)
        hots = []
        for k in range(ep):
            q = (ep - k) % ep
            hots.append((place == slot_row[q, :, low:high]).astype(f32).astype(bf16))
        with scope(f"zwait{c}"):
            if piece(need, c).size:
                rows_c = piece(need, c)
                whole(near.at[1:, rows_c, :], z_send.at[0], z_recv.at[c]).wait_recv()
        with scope(f"pick{c}"):
            total = jnp.zeros((size, width), f32)
            for k in range(ep):
                block = tok[low:high, :] if k == 0 else near[k, low:high, :]
                total = total + jnp.dot(hots[k], block, preferred_element_type=f32)
            full[t, span(c), :] = (total * gain[...]).astype(bf16)
            for s in (6, 2, 4, 1) if c in AG_ACROSS else (2, 4, 1):
                ag_copy(c, s).start()
            diagonal = lax.broadcasted_iota(jnp.int32, (size, size), 0) == (
                lax.broadcasted_iota(jnp.int32, (size, size), 1)
            )
            squares = jnp.sum(total * total, axis=1, keepdims=True)
            square_row[c, 0, :, :size] = jnp.sum(
                jnp.where(diagonal, squares, 0.0), axis=0, keepdims=True
            )
            for m in range(1, tp):
                square_copy(c, m).start()

    def forward(c, stages):
        with scope(f"fwd{c}_{stages[0][0]}"):
            for s, onward in stages:
                ag_wait(c, s)
                for after in onward:
                    ag_copy(c, after).start()

    first = ((2, (6, 3)), (4, (8, 5)))
    second = ((6, (7,)), (8, (9,)))

    sums = (
        (2, 0, 0, 2), (4, 1, 0, 4), (6, 0, 1, 2), (6, 1, 1, 4), (4, 0, 2, 4), (2, 1, 2, 2),
    )

    def r1_copy(c, i):
        return remote(
            part.at[2 * i + 1, span(c), :], got1.at[i, span(c), :],
            r1_send.at[0], r1_recv.at[c, int(i == 3)], me, flip(1),
        )

    def r2_copy(c, s):
        m, part_of, slot, to = sums[s]
        rows_h = part_rows(c, part_of)
        return remote(
            part.at[m, rows_h, :], got2.at[slot, rows_h, :],
            r2_send.at[0], r2_recv.at[c, {2: 1, 3: 2}.get(s, 0)], me, flip(to),
        )

    tile = min(ff, 256)

    scales = {}

    def gate_up(c):
        gate_up_first(c)
        gate_up_rest(c)

    def gate_up_first(c):
        gathered(c)
        with scope(f"gateup{c}"):
            gate_up_tiles(c, range(ff // tile // 2))

    def gate_up_rest(c):
        with scope(f"gaterest{c}"):
            gate_up_tiles(c, range(ff // tile // 2, ff // tile))

    def gathered(c):
        with scope(f"agwait{c}"):
            whole(full.at[: tp // 2, span(c), :], ag_send.at[0], ag_recv.at[c, 0]).wait_recv()
            whole(square_row.at[c, 1:], s_send.at[0], s_recv.at[c]).wait_recv()
        with scope(f"scale{c}"):
            size = sizes[c]
            diagonal = lax.broadcasted_iota(jnp.int32, (size, size), 0) == (
                lax.broadcasted_iota(jnp.int32, (size, size), 1)
            )
            squares = square_row[c, 0, :, :size]
            for m in range(1, tp):
                squares = squares + square_row[c, m, :, :size]
            squares = jnp.sum(jnp.where(diagonal, squares, 0.0), axis=1, keepdims=True)
            scales[c] = lax.rsqrt(squares / d + EPS)

    def gate_up_tiles(c, tiles):
        for j in tiles:
            units = slice(j * tile, (j + 1) * tile)
            gate = jnp.zeros((sizes[c], tile), f32)
            upward = jnp.zeros((sizes[c], tile), f32)
            for b in range(tp):
                at = slice(b * width, (b + 1) * width)
                gate = gate + jnp.dot(
                    full[b, span(c), :], wg[at, units], preferred_element_type=f32
                )
                upward = upward + jnp.dot(
                    full[b, span(c), :], wu[at, units], preferred_element_type=f32
                )
            gate, upward = gate * scales[c], upward * scales[c]
            hidden[c % 2, : sizes[c], units] = (
                gate / (1.0 + jnp.exp(-gate)) * upward
            ).astype(bf16)

    def down(c):
        def block(m):
            return jnp.dot(
                hidden[c % 2, : sizes[c], :], wd[:, cols(m)], preferred_element_type=f32
            )

        with scope(f"odd{c}"):
            for m in evens:
                part[m + 1, span(c), :] = block(m + 1).astype(bf16)
            if c == chunks - 1:
                for m in evens:
                    r1_copy(c, m // 2).start()
        with scope(f"even{c}"):
            for m in evens:
                sums_even[m // 2, span(c), :] = block(m)
            if c < chunks - 1:
                for m in evens:
                    r1_copy(c, m // 2).start()

    def sum_copy(c, m):
        return remote(
            part.at[m, span(c), :], got2.at[m // 2 - 1, span(c), :],
            r2_send.at[0], r2_recv.at[c, 0], me, flip(m),
        )

    def reduce(c):
        half = sizes[c] // 2
        with scope(f"reduce{c}"):
            for m in evens:
                if m == 6:
                    whole(got1.at[3, span(c), :], r1_send.at[0], r1_recv.at[c, 1]).wait_recv()
                elif m == 2:
                    whole(got1.at[:3, span(c), :], r1_send.at[0], r1_recv.at[c, 0]).wait_recv()
                mine = sums_even[m // 2, span(c), :] + got1[m // 2, span(c), :].astype(f32)
                if m and c in SUM_ACROSS:
                    part[m, span(c), :] = mine.astype(bf16)
                    sum_copy(c, m).start()
                elif m == 6:
                    part[6, span(c), :] = mine.astype(bf16)
                    r2_copy(c, 2).start()
                    r2_copy(c, 3).start()
                elif m:
                    part_of = 0 if m == 2 else 1
                    sent, kept = part_of * half, (1 - part_of) * half
                    part[m, part_rows(c, part_of), :] = mine[sent : sent + half].astype(bf16)
                    r2_copy(c, part_of).start()
                    keep[part_rows(c, 1 - part_of), :] = mine[kept : kept + half]
                else:
                    own[span(c), :] = mine

    def relay(c):
        if c in SUM_ACROSS:
            return
        with scope(f"relay{c}"):
            for s, m, part_of in ((2, 4, 0), (3, 2, 1)):
                rows_h = part_rows(c, part_of)
                r2_copy(c, s).wait_recv()
                part[m, rows_h, :] = (
                    keep[rows_h, :] + got2[1, rows_h, :].astype(f32)
                ).astype(bf16)
                r2_copy(c, s + 2).start()

    def finish(c):
        rows_c = piece(done, c)
        low = max(0, (starts[c] - spare) // LANES * LANES)
        hots = []
        if rows_c.size:
            place = lax.broadcasted_iota(jnp.int32, (rows_c.size, ends[c] - low), 1) + low
            for k in range(ep):
                hots.append(
                    (slot_col[k, rows_c, :] == place.astype(f32)).astype(f32).astype(bf16)
                )
        with scope(f"sumwait{c}"):
            whole(got2.at[: 3 if c in SUM_ACROSS else 2, span(c), :], r2_send.at[0], r2_recv.at[c, 0]).wait_recv()
        with scope(f"finish{c}"):
            at = span(c)
            total = own[at, :] + got2[0, at, :].astype(f32) + got2[2, at, :].astype(f32)
            if c in SUM_ACROSS:
                total = total + got2[1, at, :].astype(f32)
            weighted[at, :] = (total * aff_col[at, :]).astype(bf16)
            if rows_c.size:
                for k in range(ep):
                    back[k, rows_c, :] = jnp.dot(
                        hots[k], weighted[low : ends[c], :], preferred_element_type=f32
                    ).astype(bf16)
                for k in hops:
                    back_copy(c, k).start()

    def back_copy(c, k):
        rows_c = piece(done, c)
        return remote(
            back.at[k, rows_c, :], got_back.at[k, rows_c, :], b_send.at[0], b_recv.at[c],
            lax.rem(me + k, ep), t,
        )

    def mix(c):
        if piece(done, c).size:
            with scope(f"mix{c}"):
                rows_c = piece(done, c)
                total = back[0, rows_c, :].astype(f32)
                whole(got_back.at[1:, rows_c, :], b_send.at[0], b_recv.at[c]).wait_recv()
                for k in range(1, ep):
                    total = total + got_back[k, rows_c, :].astype(f32)
                out[rows_c, :] = total.astype(bf16)

    def fwd_a(c):
        forward(c, ((2, (3,)), (4, (5,))) if c in AG_ACROSS else first)

    def fwd_b(c):
        forward(c, ((6, (7,)),) if c in AG_ACROSS else second)

    def wait_weights(c):
        with scope("wwait"):
            weights[c].wait()

    steps = {
        "pick": pick, "A": fwd_a, "B": fwd_b, "gu": gate_up, "ga": gate_up_first, "gb": gate_up_rest, "dn": down, "red": reduce,
        "rel": relay, "fin": finish, "mix": mix, "w": wait_weights, "z": z_start,
    }
    for name, c in ORDER:
        steps[name](c)

    with scope("tail"):
        for ref, send, recv in (
            (square_row.at[:, 1:], s_send, s_recv),
            (near.at[1:], z_send, s_recv),
            (got_back.at[1:], b_send, s_recv),
            (full.at[: tp - 1], ag_send, s_recv),
            (got2, r2_send, s_recv),
            (got1, r1_send, s_recv),
        ):
            whole(ref, send.at[0], recv.at[0]).wait_send()


ORDER = (
    ("z", 1), ("pick", 0), ("z", 2), ("pick", 1), ("z", 3), ("A", 0), ("B", 0), ("pick", 2),
    ("pick", 3), ("w", 0), ("w", 1), ("gu", 0), ("A", 1), ("B", 1), ("w", 2), ("dn", 0), ("ga", 1),
    ("A", 2), ("B", 2), ("red", 0), ("gb", 1), ("dn", 1), ("ga", 2), ("red", 1), ("gb", 2),
    ("A", 3), ("B", 3), ("dn", 2), ("ga", 3), ("red", 2), ("gb", 3), ("dn", 3), ("fin", 0),
    ("red", 3), ("fin", 1), ("fin", 2), ("fin", 3), ("rel", 0), ("rel", 1), ("rel", 2), ("rel", 3),
    ("mix", 0), ("mix", 1), ("mix", 2), ("mix", 3),
)


def fused(ep, tp, tokens, norm_gain, chosen, affinity, w_gate, w_up, w_down):
    tok_dev, width = tokens.shape
    d, ff = w_gate.shape[1:]
    count = chosen.shape[1]
    rows = -(-count // 8) * 8
    size = -(-count // (32 * len(SHARES))) * 32
    sizes = (size,) * (len(SHARES) - 1) + (rows - size * (len(SHARES) - 1),)
    largest = max(sizes)
    f32, bf16 = jnp.float32, jnp.bfloat16
    vmem = pl.BlockSpec(memory_space=pltpu.VMEM)
    hbm = pl.BlockSpec(memory_space=pl.ANY)
    dma = pltpu.SemaphoreType.DMA
    return pl.pallas_call(
        functools.partial(kernel, ep, tp, sizes),
        out_shape=pltpu.VMEM((tok_dev, width), bf16),
        in_specs=[hbm] * 7,
        out_specs=vmem,
        scratch_shapes=[
            pltpu.VMEM((tok_dev, width), bf16),
            pltpu.VMEM((1, width), f32),
            pltpu.VMEM((1, count), jnp.int32),
            pltpu.VMEM((1, count), f32),
            pltpu.VMEM((d, ff), bf16),
            pltpu.VMEM((d, ff), bf16),
            pltpu.VMEM((ff, d), bf16),
            pltpu.VMEM((tp, rows, width), bf16),
            pltpu.VMEM((2, largest, ff), bf16),
            pltpu.VMEM((tp, rows, width), bf16),
            pltpu.VMEM((tp // 2, rows, width), bf16),
            pltpu.VMEM((3, rows, width), bf16),
            pltpu.VMEM((tp // 2, rows, width), f32),
            pltpu.VMEM((rows, width), f32),
            pltpu.VMEM((rows, width), bf16),
            pltpu.VMEM((ep, tok_dev, width), bf16),
            pltpu.VMEM((ep, tok_dev, width), bf16),
            pltpu.VMEM((ep, tok_dev, width), bf16),
            pltpu.VMEM((1, rows), f32),
            pltpu.VMEM((1, rows), f32),
            pltpu.VMEM((ep, 1, tok_dev), f32),
            pltpu.VMEM((ep, tok_dev, 1), f32),
            pltpu.VMEM((rows, 1), f32),
            pltpu.VMEM((len(SHARES), tp, 1, -(-largest // LANES) * LANES), f32),
            pltpu.VMEM((rows, width), f32),
            dma((4,)),
            dma((3,)),
            dma((1,)),
            dma((len(SHARES),)),
            dma((1,)),
            dma((len(SHARES),)),
            dma((1,)),
            dma((len(SHARES), 5)),
            dma((1,)),
            dma((len(SHARES), 2)),
            dma((1,)),
            dma((len(SHARES), 3)),
            dma((1,)),
            dma((len(SHARES),)),
        ],
        compiler_params=pltpu.CompilerParams(
            collective_id=0, has_side_effects=True, vmem_limit_bytes=VMEM_BYTES - 2**20
        ),
    )(tokens, norm_gain[None, :], chosen, affinity, w_gate, w_up, w_down)


EPS = 1e-06


def plain(tokens, norm_gain, chosen, affinity, w_gate, w_up, w_down):
    tok_dev, width_part = tokens.shape
    ep_count = lax.axis_size("ep")
    floats = tokens.astype(jnp.float32)
    square_sum = lax.psum(jnp.sum(floats * floats, axis=1), "tp")
    normed = (floats * lax.rsqrt(square_sum / w_gate.shape[1] + EPS)[:, None] * norm_gain[None, :]).astype(
        jnp.bfloat16
    )
    own_choice = chosen[0]
    chosen_count = own_choice.shape[0]
    bound_rows = min(tok_dev, 2 * chosen_count // ep_count)
    slot_ids = jnp.arange(bound_rows, dtype=jnp.int32)
    positions = jnp.arange(chosen_count, dtype=jnp.int32)
    every_token = lax.all_gather(normed, "ep", axis=0, tiled=True)
    picked = every_token[own_choice]
    piece = lax.all_gather(picked, "tp", axis=1, tiled=True)
    gate_rows = w_gate[0]
    up_rows = w_up[0]
    gate = jnp.dot(piece, gate_rows, preferred_element_type=jnp.float32)
    upward = jnp.dot(piece, up_rows, preferred_element_type=jnp.float32)
    hidden = (jax.nn.silu(gate) * upward).astype(jnp.bfloat16)
    columns = w_down[0]
    summed = lax.psum_scatter(
        lax.dot_general(
            columns, hidden, (((0,), (1,)), ((), ())), preferred_element_type=jnp.float32
        ).astype(jnp.bfloat16),
        "tp",
        scatter_dimension=0,
        tiled=True,
    ).astype(jnp.float32)
    weighted = (summed * affinity[0][None, :]).astype(jnp.bfloat16).T
    owner = own_choice // tok_dev
    owner_local = own_choice - owner * tok_dev
    owner_hot = owner[:, None] == jnp.arange(ep_count, dtype=jnp.int32)[None, :]
    running = jnp.cumsum(owner_hot.astype(jnp.int32), axis=0)
    place = jnp.sum(jnp.where(owner_hot, running, 0), axis=1) - 1
    back_match = owner_hot.T[:, None, :] & (place[None, None, :] == slot_ids[None, :, None])
    back_filled = jnp.any(back_match, axis=2)
    back_pick = jnp.sum(jnp.where(back_match, positions[None, None, :], 0), axis=2)
    back_rows = jnp.where(back_filled[..., None], weighted[back_pick], jnp.zeros((), jnp.bfloat16))
    back_token = jnp.where(back_filled, owner_local[back_pick], tok_dev)
    got_back, got_token = (
        lax.all_to_all(back_rows, "ep", split_axis=0, concat_axis=0, tiled=True),
        lax.all_to_all(back_token, "ep", split_axis=0, concat_axis=0, tiled=True),
    )
    total = jnp.zeros((tok_dev, width_part), jnp.float32)
    total = total.at[got_token.reshape(-1)].add(
        got_back.reshape(-1, width_part).astype(jnp.float32), mode="drop"
    )
    return total.astype(jnp.bfloat16)


def solution(mesh):
    ep, tp = mesh.shape["ep"], mesh.shape["tp"]

    def local(tokens, *rest):
        whole_lanes = tokens.shape[1] % LANES == 0 and rest[3].shape[2] % LANES == 0
        if whole_lanes and tp == 2**3:
            return fused(ep, tp, tokens, *rest)
        return plain(tokens, *rest)

    in_specs = (
        P("ep", "tp"),
        P("tp"),
        P("ep", None),
        P("ep", None),
        P("ep", None, "tp"),
        P("ep", None, "tp"),
        P("ep", "tp", None),
    )
    out_specs = P("ep", "tp")
    return jax.shard_map(local, mesh=mesh, in_specs=in_specs, out_specs=out_specs, check_vma=False)
```

```python
import functools

import jax
import jax.numpy as jnp
from jax import lax
from jax.experimental import pallas as pl
from jax.experimental.pallas import tpu as pltpu
from jax.sharding import PartitionSpec as P

MESH = pl.DeviceIdType.MESH
VMEM_BYTES = 67_043_328
LANES = 128
SHARES = (1, 1, 1, 1)
AG_ACROSS = (0, 1, 2, 3)
SUM_ACROSS = (0, 1, 2, 3)


def kernel(
    ep, tp, sizes,
    tok_hbm, gain_hbm, chosen_hbm, aff_hbm, wg_hbm, wu_hbm, wd_hbm,
    out,
    tok, gain, chosen, aff, wg, wu, wd, full, hidden, part, got1, got2, sums_even, own, weighted,
    near, back, got_back, chosen_row, aff_row, slot_row, slot_col,
    aff_col, square_row, keep, in_sem, w_sem, s_send, s_recv, z_send, z_recv, ag_send, ag_recv,
    r1_send, r1_recv, r2_send, r2_recv, b_send, b_recv,
):
    me = lax.axis_index("ep")
    t = lax.axis_index("tp")
    tok_dev, width = tok.shape
    rows = full.shape[1]
    d = wg.shape[0]
    count = chosen.shape[1]
    ff = wg.shape[1]
    chunks = len(sizes)
    starts = [sum(sizes[:c]) for c in range(chunks)]
    ends = [sum(sizes[: c + 1]) for c in range(chunks)]
    f32, bf16 = jnp.float32, jnp.bfloat16
    scope = jax.named_scope

    def flip(m):
        index, bit = t, 1
        while bit <= m:
            if m & bit:
                index = index + bit - 2 * bit * ((t // bit) % 2)
            bit *= 2
        return index

    def cols(m):
        return pl.ds(pl.multiple_of(flip(m) * width, LANES), width)

    def remote(src, dst, send, recv, ep_to, tp_to):
        return pltpu.make_async_remote_copy(
            src_ref=src, dst_ref=dst, send_sem=send, recv_sem=recv,
            device_id=(ep_to, tp_to), device_id_type=MESH,
        )

    def whole(ref, send, recv):
        return remote(ref, ref, send, recv, me, flip(1))

    evens = [6, 2, 4, 0]
    order = list(range(chunks))
    weights = [
        pltpu.make_async_copy(h.at[0], v, w_sem.at[i])
        for i, (h, v) in enumerate(((wg_hbm, wg), (wu_hbm, wu), (wd_hbm, wd)))
    ]
    inputs = [
        pltpu.make_async_copy(h, v, in_sem.at[i])
        for i, (h, v) in enumerate(
            ((tok_hbm, tok), (gain_hbm, gain), (chosen_hbm, chosen), (aff_hbm, aff))
        )
    ]
    for copy in inputs:
        copy.start()

    spare = ep * tok_dev - count
    need = [min(tok_dev, -(-(-(-(ends[c] + spare) // ep)) // 16) * 16) for c in order]
    need[-1] = tok_dev
    least = [starts[c] // ep // 16 * 16 for c in order]
    done = [min(tok_dev, ends[c] // ep // 16 * 16) for c in order]
    done[-1] = tok_dev

    def piece(stops, c):
        start = stops[c - 1] if c else 0
        return pl.ds(start, stops[c] - start)

    barrier = pltpu.get_barrier_semaphore()
    for m in range(1, tp):
        pl.semaphore_signal(barrier, inc=1, device_id=(me, flip(m)), device_id_type=MESH)
    for k in range(1, ep):
        pl.semaphore_signal(
            barrier, inc=1, device_id=(lax.rem(me + k, ep), t), device_id_type=MESH
        )
    with scope("inputs"):
        for copy in inputs:
            copy.wait()
    for copy in weights:
        copy.start()
    with scope("barrier"):
        pl.semaphore_wait(barrier, tp + ep - 2)

    def z_copy(c, k):
        rows_c = piece(need, c)
        return remote(
            tok.at[rows_c, :], near.at[k, rows_c, :], z_send.at[0], z_recv.at[c],
            lax.rem(me + k, ep), t,
        )

    def farthest_first():
        after, before = ep - 1 - me, me
        longer = (after - before + ep) // ep
        gap = (2 * longer - 1) * (after - before)
        short = (ep - 1 - gap) // 2
        steps = []
        for i in range(ep - 1):
            alone = (gap - 1 - i + ep) // ep
            far = longer * (ep - 1 - i) + (1 - longer) * i
            pair = i - gap
            near_by = me + (1 - 2 * ((pair + 2 * ep) % 2)) * (short - (pair + 2 * ep) // 2 + ep)
            to = alone * far + (1 - alone) * near_by
            steps.append(lax.rem(to - me + ep, ep))
        return steps

    hops = farthest_first()
    hops = hops[:1] + hops[:0:-1]

    def z_start(c):
        if piece(need, c).size:
            for k in hops:
                z_copy(c, k).start()

    z_start(0)

    with scope("index"):
        chosen_row[...] = jnp.full(chosen_row.shape, -1.0, f32)
        aff_row[...] = jnp.zeros(aff_row.shape, f32)
        chosen_row[:, :count] = chosen[...].astype(f32)
        aff_row[:, :count] = aff[...]
        diagonal = lax.broadcasted_iota(jnp.int32, (rows, rows), 0) == lax.broadcasted_iota(
            jnp.int32, (rows, rows), 1
        )
        given = jnp.sum(jnp.where(diagonal, chosen_row[...], 0.0), axis=1, keepdims=True)
        factor = jnp.sum(jnp.where(diagonal, aff_row[...], 0.0), axis=1, keepdims=True)

        owners = [lax.rem(me + q, ep) for q in range(ep)]
        lane = lax.broadcasted_iota(jnp.int32, (rows, tok_dev), 1)
        sub = lax.broadcasted_iota(jnp.int32, (tok_dev, rows), 0)
        taken_row, taken_col, aff_token = [], [], []
        for q in range(ep):
            match = given == (lane + owners[q] * tok_dev).astype(f32)
            taken_row.append(jnp.sum(match.astype(f32), axis=0, keepdims=True))
            aff_token.append(jnp.sum(jnp.where(match, factor, 0.0), axis=0, keepdims=True))
            match = chosen_row[...] == (sub + owners[q] * tok_dev).astype(f32)
            taken_col.append(jnp.sum(match.astype(f32), axis=1, keepdims=True))
        down_index = lax.broadcasted_iota(jnp.int32, (tok_dev, tok_dev), 0) * ep
        across_index = lax.broadcasted_iota(jnp.int32, (tok_dev, tok_dev), 1) * ep
        place_all = lax.broadcasted_iota(jnp.int32, (rows, tok_dev), 0).astype(f32)
        factor_sum = jnp.zeros((rows, tok_dev), f32)
        for q in range(ep):
            ahead = jnp.zeros((tok_dev, tok_dev), f32)
            above = jnp.zeros((tok_dev, tok_dev), f32)
            for p in range(ep):
                ahead = ahead + jnp.where(
                    down_index + owners[p] < across_index + owners[q], taken_col[p], 0.0
                )
                above = above + jnp.where(
                    across_index + owners[p] < down_index + owners[q], taken_row[p], 0.0
                )
            slot_row[q] = jnp.where(
                taken_row[q] > 0, jnp.sum(ahead, axis=0, keepdims=True), -1.0
            )
            slot_col[q] = jnp.where(
                taken_col[q] > 0, jnp.sum(above, axis=1, keepdims=True), -1.0
            )
            factor_sum = factor_sum + jnp.where(place_all == slot_row[q], aff_token[q], 0.0)
        aff_col[...] = jnp.sum(factor_sum, axis=1, keepdims=True)

    def span(c):
        return pl.ds(starts[c], sizes[c])

    def part_rows(c, part_of):
        half = sizes[c] // 2
        return pl.ds(starts[c] + part_of * half, half)

    routes = {
        1: (0, None, 1), 2: (0, None, 2), 4: (0, None, 4),
        3: (2, None, 1), 6: (2, 0, 4), 5: (4, None, 1), 8: (4, 1, 2),
        7: (6, 0, 1), 9: (6, 1, 1),
    }

    across = {
        1: (0, None, 1), 2: (0, None, 2), 4: (0, None, 4), 6: (0, None, 6),
        3: (2, None, 1), 5: (4, None, 1), 7: (6, None, 1),
    }
    ag_slot = {2: 1, 4: 2, 6: 3, 8: 4, 1: 0, 3: 0, 5: 0, 7: 0, 9: 0}

    def route(c, s):
        return (across if c in AG_ACROSS else routes)[s]

    def ag_block(c, m, part_of):
        return full.at[flip(m), span(c) if part_of is None else part_rows(c, part_of), :]

    def ag_copy(c, s):
        m, part_of, to = route(c, s)
        block = ag_block(c, m, part_of)
        return remote(block, block, ag_send.at[0], ag_recv.at[c, ag_slot[s]], me, flip(to))

    def ag_wait(c, s):
        m, part_of, to = route(c, s)
        block = ag_block(c, m ^ to, part_of)
        whole(block, ag_send.at[0], ag_recv.at[c, ag_slot[s]]).wait_recv()

    def square_copy(c, m):
        return remote(
            square_row.at[c, 0], square_row.at[c, m], s_send.at[0], s_recv.at[c], me, flip(m)
        )

    def pick(c):
        low, high, size = least[c], need[c], sizes[c]
        place = (
            lax.broadcasted_iota(jnp.int32, (size, high - low), 0) + starts[c]
        ).astype(f32)
        hots = []
        for k in range(ep):
            q = (ep - k) % ep
            hots.append((place == slot_row[q, :, low:high]).astype(f32).astype(bf16))
        with scope(f"zwait{c}"):
            if piece(need, c).size:
                rows_c = piece(need, c)
                whole(near.at[1:, rows_c, :], z_send.at[0], z_recv.at[c]).wait_recv()
        with scope(f"pick{c}"):
            total = jnp.zeros((size, width), f32)
            for k in range(ep):
                block = tok[low:high, :] if k == 0 else near[k, low:high, :]
                total = total + jnp.dot(hots[k], block, preferred_element_type=f32)
            full[t, span(c), :] = (total * gain[...]).astype(bf16)
            for s in (6, 2, 4, 1) if c in AG_ACROSS else (2, 4, 1):
                ag_copy(c, s).start()
            diagonal = lax.broadcasted_iota(jnp.int32, (size, size), 0) == (
                lax.broadcasted_iota(jnp.int32, (size, size), 1)
            )
            squares = jnp.sum(total * total, axis=1, keepdims=True)
            square_row[c, 0, :, :size] = jnp.sum(
                jnp.where(diagonal, squares, 0.0), axis=0, keepdims=True
            )
            for m in range(1, tp):
                square_copy(c, m).start()

    def forward(c, stages):
        with scope(f"fwd{c}_{stages[0][0]}"):
            for s, onward in stages:
                ag_wait(c, s)
                for after in onward:
                    ag_copy(c, after).start()

    first = ((2, (6, 3)), (4, (8, 5)))
    second = ((6, (7,)), (8, (9,)))

    sums = (
        (2, 0, 0, 2), (4, 1, 0, 4), (6, 0, 1, 2), (6, 1, 1, 4), (4, 0, 2, 4), (2, 1, 2, 2),
    )

    def r1_copy(c, i):
        return remote(
            part.at[2 * i + 1, span(c), :], got1.at[i, span(c), :],
            r1_send.at[0], r1_recv.at[c, int(i == 3)], me, flip(1),
        )

    def r2_copy(c, s):
        m, part_of, slot, to = sums[s]
        rows_h = part_rows(c, part_of)
        return remote(
            part.at[m, rows_h, :], got2.at[slot, rows_h, :],
            r2_send.at[0], r2_recv.at[c, {2: 1, 3: 2}.get(s, 0)], me, flip(to),
        )

    tile = min(ff, 256)

    scales = {}

    def gate_up(c):
        gate_up_first(c)
        gate_up_rest(c)

    def gate_up_first(c):
        gathered(c)
        with scope(f"gateup{c}"):
            gate_up_tiles(c, range(ff // tile // 2))

    def gate_up_rest(c):
        with scope(f"gaterest{c}"):
            gate_up_tiles(c, range(ff // tile // 2, ff // tile))

    def gathered(c):
        with scope(f"agwait{c}"):
            whole(full.at[: tp // 2, span(c), :], ag_send.at[0], ag_recv.at[c, 0]).wait_recv()
            whole(square_row.at[c, 1:], s_send.at[0], s_recv.at[c]).wait_recv()
        with scope(f"scale{c}"):
            size = sizes[c]
            diagonal = lax.broadcasted_iota(jnp.int32, (size, size), 0) == (
                lax.broadcasted_iota(jnp.int32, (size, size), 1)
            )
            squares = square_row[c, 0, :, :size]
            for m in range(1, tp):
                squares = squares + square_row[c, m, :, :size]
            squares = jnp.sum(jnp.where(diagonal, squares, 0.0), axis=1, keepdims=True)
            scales[c] = lax.rsqrt(squares / d + EPS)

    def gate_up_tiles(c, tiles):
        for j in tiles:
            units = slice(j * tile, (j + 1) * tile)
            gate = jnp.zeros((sizes[c], tile), f32)
            upward = jnp.zeros((sizes[c], tile), f32)
            for b in range(tp):
                at = slice(b * width, (b + 1) * width)
                gate = gate + jnp.dot(
                    full[b, span(c), :], wg[at, units], preferred_element_type=f32
                )
                upward = upward + jnp.dot(
                    full[b, span(c), :], wu[at, units], preferred_element_type=f32
                )
            gate, upward = gate * scales[c], upward * scales[c]
            hidden[c % 2, : sizes[c], units] = (
                gate / (1.0 + jnp.exp(-gate)) * upward
            ).astype(bf16)

    def down(c):
        def block(m):
            return jnp.dot(
                hidden[c % 2, : sizes[c], :], wd[:, cols(m)], preferred_element_type=f32
            )

        with scope(f"odd{c}"):
            for m in evens:
                part[m + 1, span(c), :] = block(m + 1).astype(bf16)
            if c == chunks - 1:
                for m in evens:
                    r1_copy(c, m // 2).start()
        with scope(f"even{c}"):
            for m in evens:
                sums_even[m // 2, span(c), :] = block(m)
            if c < chunks - 1:
                for m in evens:
                    r1_copy(c, m // 2).start()

    def sum_copy(c, m):
        return remote(
            part.at[m, span(c), :], got2.at[m // 2 - 1, span(c), :],
            r2_send.at[0], r2_recv.at[c, 0], me, flip(m),
        )

    def reduce(c):
        half = sizes[c] // 2
        with scope(f"reduce{c}"):
            for m in evens:
                if m == 6:
                    whole(got1.at[3, span(c), :], r1_send.at[0], r1_recv.at[c, 1]).wait_recv()
                elif m == 2:
                    whole(got1.at[:3, span(c), :], r1_send.at[0], r1_recv.at[c, 0]).wait_recv()
                mine = sums_even[m // 2, span(c), :] + got1[m // 2, span(c), :].astype(f32)
                if m and c in SUM_ACROSS:
                    part[m, span(c), :] = mine.astype(bf16)
                    sum_copy(c, m).start()
                elif m == 6:
                    part[6, span(c), :] = mine.astype(bf16)
                    r2_copy(c, 2).start()
                    r2_copy(c, 3).start()
                elif m:
                    part_of = 0 if m == 2 else 1
                    sent, kept = part_of * half, (1 - part_of) * half
                    part[m, part_rows(c, part_of), :] = mine[sent : sent + half].astype(bf16)
                    r2_copy(c, part_of).start()
                    keep[part_rows(c, 1 - part_of), :] = mine[kept : kept + half]
                else:
                    own[span(c), :] = mine

    def relay(c):
        if c in SUM_ACROSS:
            return
        with scope(f"relay{c}"):
            for s, m, part_of in ((2, 4, 0), (3, 2, 1)):
                rows_h = part_rows(c, part_of)
                r2_copy(c, s).wait_recv()
                part[m, rows_h, :] = (
                    keep[rows_h, :] + got2[1, rows_h, :].astype(f32)
                ).astype(bf16)
                r2_copy(c, s + 2).start()

    def finish(c):
        rows_c = piece(done, c)
        low = max(0, (starts[c] - spare) // LANES * LANES)
        hots = []
        if rows_c.size:
            place = lax.broadcasted_iota(jnp.int32, (rows_c.size, ends[c] - low), 1) + low
            for k in range(ep):
                hots.append(
                    (slot_col[k, rows_c, :] == place.astype(f32)).astype(f32).astype(bf16)
                )
        with scope(f"sumwait{c}"):
            whole(got2.at[: 3 if c in SUM_ACROSS else 2, span(c), :], r2_send.at[0], r2_recv.at[c, 0]).wait_recv()
        with scope(f"finish{c}"):
            at = span(c)
            total = own[at, :] + got2[0, at, :].astype(f32) + got2[2, at, :].astype(f32)
            if c in SUM_ACROSS:
                total = total + got2[1, at, :].astype(f32)
            weighted[at, :] = (total * aff_col[at, :]).astype(bf16)
            if rows_c.size:
                for k in range(ep):
                    back[k, rows_c, :] = jnp.dot(
                        hots[k], weighted[low : ends[c], :], preferred_element_type=f32
                    ).astype(bf16)
                for k in farthest_first():
                    back_copy(c, k).start()

    def back_copy(c, k):
        rows_c = piece(done, c)
        return remote(
            back.at[k, rows_c, :], got_back.at[k, rows_c, :], b_send.at[0], b_recv.at[c],
            lax.rem(me + k, ep), t,
        )

    def mix(c):
        if piece(done, c).size:
            with scope(f"mix{c}"):
                rows_c = piece(done, c)
                total = back[0, rows_c, :].astype(f32)
                whole(got_back.at[1:, rows_c, :], b_send.at[0], b_recv.at[c]).wait_recv()
                for k in range(1, ep):
                    total = total + got_back[k, rows_c, :].astype(f32)
                out[rows_c, :] = total.astype(bf16)

    def fwd_a(c):
        forward(c, ((2, (3,)), (4, (5,))) if c in AG_ACROSS else first)

    def fwd_b(c):
        forward(c, ((6, (7,)),) if c in AG_ACROSS else second)

    def wait_weights(c):
        with scope("wwait"):
            weights[c].wait()

    steps = {
        "pick": pick, "A": fwd_a, "B": fwd_b, "gu": gate_up, "ga": gate_up_first, "gb": gate_up_rest, "dn": down, "red": reduce,
        "rel": relay, "fin": finish, "mix": mix, "w": wait_weights, "z": z_start,
    }
    for name, c in ORDER:
        steps[name](c)

    with scope("tail"):
        for ref, send, recv in (
            (square_row.at[:, 1:], s_send, s_recv),
            (near.at[1:], z_send, s_recv),
            (got_back.at[1:], b_send, s_recv),
            (full.at[: tp - 1], ag_send, s_recv),
            (got2, r2_send, s_recv),
            (got1, r1_send, s_recv),
        ):
            whole(ref, send.at[0], recv.at[0]).wait_send()


ORDER = (
    ("z", 1), ("pick", 0), ("z", 2), ("pick", 1), ("z", 3), ("A", 0), ("B", 0), ("pick", 2),
    ("pick", 3), ("w", 0), ("w", 1), ("gu", 0), ("A", 1), ("B", 1), ("w", 2), ("dn", 0), ("ga", 1),
    ("A", 2), ("B", 2), ("red", 0), ("gb", 1), ("dn", 1), ("ga", 2), ("red", 1), ("gb", 2),
    ("A", 3), ("B", 3), ("dn", 2), ("ga", 3), ("red", 2), ("gb", 3), ("dn", 3), ("fin", 0),
    ("red", 3), ("fin", 1), ("fin", 2), ("fin", 3), ("rel", 0), ("rel", 1), ("rel", 2), ("rel", 3),
    ("mix", 0), ("mix", 1), ("mix", 2), ("mix", 3),
)


def fused(ep, tp, tokens, norm_gain, chosen, affinity, w_gate, w_up, w_down):
    tok_dev, width = tokens.shape
    d, ff = w_gate.shape[1:]
    count = chosen.shape[1]
    rows = -(-count // 8) * 8
    size = -(-count // (32 * len(SHARES))) * 32
    sizes = (size,) * (len(SHARES) - 1) + (rows - size * (len(SHARES) - 1),)
    largest = max(sizes)
    f32, bf16 = jnp.float32, jnp.bfloat16
    vmem = pl.BlockSpec(memory_space=pltpu.VMEM)
    hbm = pl.BlockSpec(memory_space=pl.ANY)
    dma = pltpu.SemaphoreType.DMA
    return pl.pallas_call(
        functools.partial(kernel, ep, tp, sizes),
        out_shape=pltpu.VMEM((tok_dev, width), bf16),
        in_specs=[hbm] * 7,
        out_specs=vmem,
        scratch_shapes=[
            pltpu.VMEM((tok_dev, width), bf16),
            pltpu.VMEM((1, width), f32),
            pltpu.VMEM((1, count), jnp.int32),
            pltpu.VMEM((1, count), f32),
            pltpu.VMEM((d, ff), bf16),
            pltpu.VMEM((d, ff), bf16),
            pltpu.VMEM((ff, d), bf16),
            pltpu.VMEM((tp, rows, width), bf16),
            pltpu.VMEM((2, largest, ff), bf16),
            pltpu.VMEM((tp, rows, width), bf16),
            pltpu.VMEM((tp // 2, rows, width), bf16),
            pltpu.VMEM((3, rows, width), bf16),
            pltpu.VMEM((tp // 2, rows, width), f32),
            pltpu.VMEM((rows, width), f32),
            pltpu.VMEM((rows, width), bf16),
            pltpu.VMEM((ep, tok_dev, width), bf16),
            pltpu.VMEM((ep, tok_dev, width), bf16),
            pltpu.VMEM((ep, tok_dev, width), bf16),
            pltpu.VMEM((1, rows), f32),
            pltpu.VMEM((1, rows), f32),
            pltpu.VMEM((ep, 1, tok_dev), f32),
            pltpu.VMEM((ep, tok_dev, 1), f32),
            pltpu.VMEM((rows, 1), f32),
            pltpu.VMEM((len(SHARES), tp, 1, -(-largest // LANES) * LANES), f32),
            pltpu.VMEM((rows, width), f32),
            dma((4,)),
            dma((3,)),
            dma((1,)),
            dma((len(SHARES),)),
            dma((1,)),
            dma((len(SHARES),)),
            dma((1,)),
            dma((len(SHARES), 5)),
            dma((1,)),
            dma((len(SHARES), 2)),
            dma((1,)),
            dma((len(SHARES), 3)),
            dma((1,)),
            dma((len(SHARES),)),
        ],
        compiler_params=pltpu.CompilerParams(
            collective_id=0, has_side_effects=True, vmem_limit_bytes=VMEM_BYTES - 2**20
        ),
    )(tokens, norm_gain[None, :], chosen, affinity, w_gate, w_up, w_down)


EPS = 1e-06


def plain(tokens, norm_gain, chosen, affinity, w_gate, w_up, w_down):
    tok_dev, width_part = tokens.shape
    ep_count = lax.axis_size("ep")
    floats = tokens.astype(jnp.float32)
    square_sum = lax.psum(jnp.sum(floats * floats, axis=1), "tp")
    normed = (floats * lax.rsqrt(square_sum / w_gate.shape[1] + EPS)[:, None] * norm_gain[None, :]).astype(
        jnp.bfloat16
    )
    own_choice = chosen[0]
    chosen_count = own_choice.shape[0]
    bound_rows = min(tok_dev, 2 * chosen_count // ep_count)
    slot_ids = jnp.arange(bound_rows, dtype=jnp.int32)
    positions = jnp.arange(chosen_count, dtype=jnp.int32)
    every_token = lax.all_gather(normed, "ep", axis=0, tiled=True)
    picked = every_token[own_choice]
    piece = lax.all_gather(picked, "tp", axis=1, tiled=True)
    gate_rows = w_gate[0]
    up_rows = w_up[0]
    gate = jnp.dot(piece, gate_rows, preferred_element_type=jnp.float32)
    upward = jnp.dot(piece, up_rows, preferred_element_type=jnp.float32)
    hidden = (jax.nn.silu(gate) * upward).astype(jnp.bfloat16)
    columns = w_down[0]
    summed = lax.psum_scatter(
        lax.dot_general(
            columns, hidden, (((0,), (1,)), ((), ())), preferred_element_type=jnp.float32
        ).astype(jnp.bfloat16),
        "tp",
        scatter_dimension=0,
        tiled=True,
    ).astype(jnp.float32)
    weighted = (summed * affinity[0][None, :]).astype(jnp.bfloat16).T
    owner = own_choice // tok_dev
    owner_local = own_choice - owner * tok_dev
    owner_hot = owner[:, None] == jnp.arange(ep_count, dtype=jnp.int32)[None, :]
    running = jnp.cumsum(owner_hot.astype(jnp.int32), axis=0)
    place = jnp.sum(jnp.where(owner_hot, running, 0), axis=1) - 1
    back_match = owner_hot.T[:, None, :] & (place[None, None, :] == slot_ids[None, :, None])
    back_filled = jnp.any(back_match, axis=2)
    back_pick = jnp.sum(jnp.where(back_match, positions[None, None, :], 0), axis=2)
    back_rows = jnp.where(back_filled[..., None], weighted[back_pick], jnp.zeros((), jnp.bfloat16))
    back_token = jnp.where(back_filled, owner_local[back_pick], tok_dev)
    got_back, got_token = (
        lax.all_to_all(back_rows, "ep", split_axis=0, concat_axis=0, tiled=True),
        lax.all_to_all(back_token, "ep", split_axis=0, concat_axis=0, tiled=True),
    )
    total = jnp.zeros((tok_dev, width_part), jnp.float32)
    total = total.at[got_token.reshape(-1)].add(
        got_back.reshape(-1, width_part).astype(jnp.float32), mode="drop"
    )
    return total.astype(jnp.bfloat16)


def solution(mesh):
    ep, tp = mesh.shape["ep"], mesh.shape["tp"]

    def local(tokens, *rest):
        whole_lanes = tokens.shape[1] % LANES == 0 and rest[3].shape[2] % LANES == 0
        if whole_lanes and tp == 2**3:
            return fused(ep, tp, tokens, *rest)
        return plain(tokens, *rest)

    in_specs = (
        P("ep", "tp"),
        P("tp"),
        P("ep", None),
        P("ep", None),
        P("ep", None, "tp"),
        P("ep", None, "tp"),
        P("ep", "tp", None),
    )
    out_specs = P("ep", "tp")
    return jax.shard_map(local, mesh=mesh, in_specs=in_specs, out_specs=out_specs, check_vma=False)
```
